32 devices in a mesh: sp: 8 (over z, core), tp: 4 (over y, x).
Axes of the slice: x: 2, y: 2, z: 4, core: 2. Of those that a mesh axis runs over, the one named last changes fastest.
Arguments:
- residual_in: bfloat16 [1024, 2048], P('sp', 'tp'), may hold values from -6 to 6
- query_wide: bfloat16 [1024, 2048], P('sp', 'tp'), may hold values from -6 to 6
- narrow_head_query: bfloat16 [1024, 1024], P('sp', 'tp'), may hold values from -6 to 6
- forget_wide: bfloat16 [1024, 2048], P('sp', 'tp'), may hold values from -6 to 6
- forget_narrow: bfloat16 [1024, 1024], P('sp', 'tp'), may hold values from -6 to 6
- room_wide: float32 [2048], P('tp'), as said below
- room_narrow: float32 [1024], P('tp'), as said below
- values: bfloat16 [1024, 2048], P('sp', 'tp'), may hold values from -6 to 6
- out_gate: bfloat16 [1024, 2048], P('sp', 'tp'), may hold values from -6 to 6
- head_gain: float32 [2048], P('tp'), may hold values from 0.1 to 1.9
- w_out: bfloat16 [2048, 2048], P(None, 'tp'), may hold values from -0.125 to 0.125
- norm_gain: float32 [2048], P('tp'), may hold values from 0.1 to 1.9
- route_ids: int32 [1024, 2], P('sp'), may hold values from 0 to 7, all different within a row; in each aligned block of 128 rows (0 to 127, 128 to 255, ...) at most 38 rows name the same one
- route_weight: float32 [1024, 2], P('sp'), may hold values from 0.25 to 1
- w_gate: bfloat16 [8, 2048, 4096], P('sp', None, 'tp'), may hold values from -0.125 to 0.125
- w_up: bfloat16 [8, 2048, 4096], P('sp', None, 'tp'), may hold values from -0.125 to 0.125
- w_down: bfloat16 [8, 4096, 2048], P('sp', 'tp'), may hold values from -0.09375 to 0.09375
Outputs:
- layer_out: bfloat16 [1024, 2048], P('sp', 'tp')
The draws below stay inside these ranges and needn't reach their ends.
Inputs may be any that keep to these rules, and one draw needn't show every extreme that they name: `room_wide`: every value is positive and below 0.125. `room_narrow`: every value is positive and below 0.125. `route_ids`: each token names 2 different experts; among the 128 tokens of one index of sp no expert is named more than 38 times, and on some indices one is named exactly 38 times.
All inputs are finite; a program needn't handle non-finite values.
Results may differ from the reference program's by a relative error of at most 0.012.
Values may be sent and summed in bfloat16 or wider, within the bound.
A program may use at most 64 MiB of HBM per device.

```python
import math
import jax
import jax.numpy as jnp
import numpy as np
from jax import lax

D = 2048
PAIRS = 16
DKW = 128
DKN = 64
DV = 64
VAL = 2048
FF = 4096
TOPK = 2
BLOCK = 64
TOK_DEV = 128
TOKENS = 1024
EXPERTS = 8
CAP = 38
N_SP = 8


def slow_heads(room_key):
    pick_key = jax.random.split(room_key, 3)[0]
    slow_share = 0.5
    return jax.random.bernoulli(pick_key, slow_share, (PAIRS, 1))


def forget_draw(key, room_key, key_dim):
    columns = PAIRS * key_dim
    noise_key, device_key, block_key, sign_key = jax.random.split(key, 4)
    noise_term = jnp.clip(jax.random.normal(noise_key, (TOKENS, columns), jnp.float32), -3.0, 3.0)
    span_count = TOKENS // TOK_DEV
    block_count = TOKENS // BLOCK
    per_device = jax.random.uniform(device_key, (span_count, 1, columns), jnp.float32, -3.0, 3.0)
    per_block = jax.random.uniform(block_key, (block_count, 1, columns), jnp.float32, -1.0, 1.0)
    offset_sum = jnp.broadcast_to(per_device, (span_count, TOK_DEV, columns)).reshape(TOKENS, columns)
    offset_sum = offset_sum + jnp.broadcast_to(per_block, (block_count, BLOCK, columns)).reshape(TOKENS, columns)
    slow_head = slow_heads(room_key)
    head_sign = jnp.where(jax.random.bernoulli(sign_key, 0.5, (PAIRS, 1)), 3.0, -3.0)
    head_shift = jnp.broadcast_to(jnp.where(slow_head, head_sign, 0.0), (PAIRS, key_dim)).reshape(1, columns)
    return jnp.clip(noise_term + offset_sum + head_shift, -6.0, 6.0).astype(jnp.bfloat16)


def room_draw(key, key_dim):
    pick_key, slow_key, fast_key = jax.random.split(key, 3)
    slow_head = slow_heads(key)
    slow_rate = jnp.exp(jax.random.uniform(slow_key, (PAIRS, key_dim), jnp.float32, math.log(0.5), math.log(2.0))) / TOKENS
    fast_rate = jnp.exp(jax.random.uniform(fast_key, (PAIRS, key_dim), jnp.float32, math.log(0.04), math.log(0.12)))
    return jnp.where(slow_head, slow_rate, fast_rate).reshape(PAIRS * key_dim).astype(jnp.float32)


def draw_forget_wide(key, part):
    return forget_draw(jax.random.fold_in(key, 11), jax.random.fold_in(key, 21), DKW)


def draw_forget_narrow(key, part):
    return forget_draw(jax.random.fold_in(key, 12), jax.random.fold_in(key, 22), DKN)


def draw_room_wide(key, part):
    return room_draw(jax.random.fold_in(key, 21), DKW)


def draw_room_narrow(key, part):
    return room_draw(jax.random.fold_in(key, 22), DKN)


def levels(stream_key, dims, cuts, least, high):
    level, own = 1.0, jax.random.fold_in(stream_key, 6)
    for dim, parts in cuts:
        heights = jnp.exp(jax.random.uniform(jax.random.fold_in(own, dim), (parts,), jnp.float32, least / len(cuts), high / len(cuts)))
        level = level * jnp.repeat(heights, dims[dim] // parts).reshape([-1 if axis == dim else 1 for axis in range(len(dims))])
    return level


def assign_block(rng, own, number, rows, number_of, top, reach, skew):
    order = jax.random.permutation(rng, number_of)
    packed, ordinary = load_shares(number_of, rows * top, reach, skew, True), load_shares(number_of, rows * top, reach, skew, False)
    places = jnp.arange(number_of)

    def named(lengths, rotation):
        used = int((lengths > 0).sum())
        fixed = max(1, used // 4)
        passed = fixed + (places - fixed + rotation * (used - fixed)) % max(1, number_of - fixed)
        return jnp.zeros((number_of,), jnp.int32).at[order[jnp.where(places < fixed, places, passed)]].set(jnp.asarray(lengths, jnp.int32))

    lengths = jnp.where(number % 4 == 0, named(packed, number // 4), named(ordinary, number - number // 4 - 1))
    mixed = jax.random.permutation(jax.random.fold_in(own, 3), number_of)
    giver, taker = mixed[0:number_of // 2 * 2:2], mixed[1:number_of // 2 * 2:2]
    margin = jnp.minimum(lengths[giver] - 1, reach - lengths[taker]) // 2
    margin = jnp.where((giver == order[0]) | (taker == order[0]) | (lengths[taker] == 0), 0, jnp.maximum(margin, 0))
    passed = jax.random.randint(jax.random.fold_in(own, 4), (number_of // 2,), 0, 1 << 20) % (margin + 1)
    lengths = lengths.at[giver].add(-passed).at[taker].add(passed)
    items = jnp.searchsorted(jnp.cumsum(lengths), jnp.arange(rows * top), side="right").astype(jnp.int32)
    listing = items.reshape(top, rows).T
    listing = listing[jax.random.permutation(jax.random.fold_in(own, 1), rows)]
    rotation = jax.random.randint(jax.random.fold_in(own, 2), (rows, 1), 0, top)
    return jnp.take_along_axis(listing, (jnp.arange(top)[None, :] + rotation) % top, axis=1)


def load_shares(amount, total, reach, skew, full):
    portions = [(1 << 20) // math.isqrt(standing ** skew) + 1 for standing in range(1, amount + 1)]
    largest = reach if full else min(reach, max(-(-total // amount), total * portions[0] // sum(portions)))
    least = 1 if total - largest >= amount - 1 else 0
    given, rest = [largest] + [least] * (amount - 1), total - largest - least * (amount - 1)
    while rest > 0:
        candidates = [i for i in range(1, amount) if given[i] < largest] or [i for i in range(1, amount) if given[i] < reach]
        mass, budget = sum([portions[i] for i in candidates]), rest
        for i in candidates:
            more = min(reach - given[i], max(1, budget * portions[i] // mass), rest)
            given[i] = given[i] + more
            rest = rest - more
    return np.array(given)


def gaussian(key, dims, deviation, bound, cuts=(), kind=jnp.bfloat16):
    result = deviation * jax.random.normal(key, dims, jnp.float32)
    if cuts:
        result = result * levels(key, dims, cuts, -0.22, 0.18)
    return jnp.clip(result, -bound, bound).astype(kind)


def setup_inputs(seed: int = 0) -> dict:
    keys = jax.random.split(jax.random.key(seed), 18)
    residual_in = gaussian(keys[0], (TOKENS, D), 1.0, 6.0, ((0, 8), (1, 4)))
    query_wide = gaussian(keys[1], (TOKENS, PAIRS * DKW), 1.0, 6.0, ((0, 8), (1, 4)))
    narrow_head_query = gaussian(keys[2], (TOKENS, PAIRS * DKN), 1.0, 6.0, ((0, 8), (1, 4)))
    forget_wide = draw_forget_wide(jax.random.fold_in(keys[17], 71), 0)
    forget_narrow = draw_forget_narrow(jax.random.fold_in(keys[17], 71), 0)
    room_wide = draw_room_wide(jax.random.fold_in(keys[17], 71), 0)
    room_narrow = draw_room_narrow(jax.random.fold_in(keys[17], 71), 0)
    values = gaussian(keys[7], (TOKENS, VAL), 1.0, 6.0, ((0, 8), (1, 4)))
    out_gate = gaussian(keys[8], (TOKENS, VAL), 1.0, 6.0, ((0, 8), (1, 4)))
    head_gain = jnp.clip(1.0 + 0.18 * jax.random.normal(keys[9], (VAL,), jnp.float32), 0.1, 1.9)
    w_out = gaussian(keys[10], (VAL, D), VAL ** -0.5, 0.125, ((1, 4),))
    norm_gain = jnp.clip(1.0 + 0.18 * jax.random.normal(keys[11], (D,), jnp.float32), 0.1, 1.9)
    route_ids_keys = jax.random.split(jax.random.fold_in(keys[12], 1), TOKENS // TOK_DEV)
    route_ids_turns = jax.random.permutation(jax.random.fold_in(keys[12], 3), TOKENS // TOK_DEV)
    route_ids = jax.vmap(lambda own, number: assign_block(jax.random.fold_in(keys[12], 2), own, number, TOK_DEV, EXPERTS, TOPK, CAP, 2))(route_ids_keys, route_ids_turns).reshape((TOKENS, TOPK))
    route_weight = jnp.clip(0.25 + 0.75 * jax.random.uniform(keys[13], (TOKENS, TOPK), jnp.float32) ** levels(keys[13], (TOKENS, TOPK), ((0, 8),), -0.2, 0.2), 0.25, 1.0)
    w_gate = gaussian(keys[14], (EXPERTS, D, FF), D ** -0.5, 0.125, ((0, 8), (2, 4)))
    w_up = gaussian(keys[15], (EXPERTS, D, FF), D ** -0.5, 0.125, ((0, 8), (2, 4)))
    w_down = gaussian(keys[16], (EXPERTS, FF, D), FF ** -0.5, 0.09375, ((0, 8), (1, 4)))
    return {"residual_in": residual_in, "query_wide": query_wide, "narrow_head_query": narrow_head_query, "forget_wide": forget_wide, "forget_narrow": forget_narrow, "room_wide": room_wide, "room_narrow": room_narrow, "values": values, "out_gate": out_gate, "head_gain": head_gain, "w_out": w_out, "norm_gain": norm_gain, "route_ids": route_ids, "route_weight": route_weight, "w_gate": w_gate, "w_up": w_up, "w_down": w_down}


EPS = 1e-06
TOP_PRECISION = lax.Precision.HIGHEST

def run_blocks(queries, rates, contents, log_decay, block_len, initial):
    length, head_count, key_dim = queries.shape
    value_dim = contents.shape[-1]
    span_count = length // block_len

    def to_spans(tensor):
        return tensor.reshape(span_count, block_len, head_count, tensor.shape[-1]).transpose(0, 2, 1, 3)
    span_query = to_spans(queries)
    span_rate = to_spans(rates)
    span_value = to_spans(contents)
    inside = jnp.cumsum(to_spans(log_decay), axis=2)
    middle = inside[:, :, block_len // 2 - 1:block_len // 2, :]
    ending = inside[:, :, block_len - 1:block_len, :]
    near_query = span_query * jnp.exp(inside - middle)
    near_rate = span_rate * jnp.exp(middle - inside)
    far_query = span_query * jnp.exp(inside)
    far_rate = span_rate * jnp.exp(ending - inside)
    fading = jnp.exp(ending[:, :, 0, :])
    causal = jnp.tril(jnp.ones((block_len, block_len), jnp.float32))

    def advance(running_total, slice_pieces):
        scores = jnp.einsum('htk,hsk->hts', slice_pieces[0], slice_pieces[1], precision=TOP_PRECISION) * causal
        final_output = jnp.einsum('hts,hsv->htv', scores, slice_pieces[4], precision=TOP_PRECISION)
        final_output = final_output + jnp.einsum('ncw,nws->ncs', slice_pieces[2], running_total, precision=TOP_PRECISION)
        running_total = slice_pieces[5][..., None] * running_total + jnp.einsum('jlg,jlq->jgq', slice_pieces[3], slice_pieces[4], precision=TOP_PRECISION)
        return (running_total, final_output)
    final, outputs = lax.scan(advance, initial, (near_query, near_rate, far_query, far_rate, span_value, fading))
    return (final, outputs.transpose(0, 2, 1, 3).reshape(length, head_count, value_dim))

def head_inputs(raw_query, raw_forget, room_vec, key_dim):
    length = raw_query.shape[0]
    activated = jax.nn.silu(raw_query.astype(jnp.float32)).reshape(length, -1, key_dim)
    in_rate = (room_vec * jax.nn.sigmoid(-raw_forget.astype(jnp.float32))).reshape(length, -1, key_dim)
    return (activated, in_rate, jnp.log1p(-in_rate))

def head_norm(outputs):
    return outputs * lax.rsqrt(lax.optimization_barrier(jnp.mean(outputs * outputs, axis=-1, keepdims=True)) + EPS)

def slot_positions(block_ids):
    matches = (block_ids[:, None] == jnp.arange(EXPERTS, dtype=jnp.int32)[None, :]).astype(jnp.int32)
    slot_rank = lax.optimization_barrier(jnp.sum((jnp.cumsum(matches, axis=0) - matches) * matches, axis=1))
    return block_ids * CAP + slot_rank

def slot_owners(positions):
    owners = jnp.full((EXPERTS * CAP,), TOK_DEV, jnp.int32)
    return owners.at[positions].set(jnp.arange(TOK_DEV * TOPK, dtype=jnp.int32) // TOPK)

def reference(residual_in, query_wide, narrow_head_query, forget_wide, forget_narrow, room_wide, room_narrow, values, out_gate, head_gain, w_out, norm_gain, route_ids, route_weight, w_gate, w_up, w_down):
    length = residual_in.shape[0]
    value_cols = values.astype(jnp.float32).reshape(length, PAIRS, 2, DV)
    wide_query, wide_rate, wide_log = head_inputs(query_wide, forget_wide, room_wide, DKW)
    narrow_query, narrow_rate, narrow_log = head_inputs(narrow_head_query, forget_narrow, room_narrow, DKN)
    _, wide_out = run_blocks(wide_query, wide_rate, value_cols[:, :, 0], wide_log, BLOCK, jnp.zeros((PAIRS, DKW, DV), jnp.float32))
    _, narrow_out = run_blocks(narrow_query, narrow_rate, value_cols[:, :, 1], narrow_log, BLOCK, jnp.zeros((PAIRS, DKN, DV), jnp.float32))
    normed_heads = jnp.stack([head_norm(wide_out), head_norm(narrow_out)], axis=2).reshape(length, VAL)
    mixed = (normed_heads * head_gain * jax.nn.silu(out_gate.astype(jnp.float32))).astype(jnp.bfloat16)
    projected = jnp.dot(mixed, w_out, preferred_element_type=jnp.float32)
    residual_mid = (residual_in.astype(jnp.float32) + projected).astype(jnp.bfloat16)
    mid_float = residual_mid.astype(jnp.float32)
    scale_rows = lax.rsqrt(lax.optimization_barrier(jnp.mean(mid_float * mid_float, axis=1, keepdims=True)) + EPS)
    token_rows = (mid_float * scale_rows * norm_gain).astype(jnp.bfloat16)
    block_ids = route_ids.reshape(N_SP, TOK_DEV * TOPK)
    positions = jax.vmap(slot_positions)(block_ids)
    owners = jax.vmap(slot_owners)(positions)
    block_start = (jnp.arange(N_SP, dtype=jnp.int32) * TOK_DEV)[:, None]
    global_owner = jnp.where(owners < TOK_DEV, owners + block_start, TOKENS).astype(jnp.int32)
    by_expert = global_owner.reshape(N_SP, EXPERTS, CAP).transpose(1, 0, 2).reshape(EXPERTS, N_SP * CAP)

    def one_expert(operands):
        gate_w, up_w, down_w, holder_index = operands
        rows_in = jnp.take(token_rows, holder_index, axis=0, mode='fill', fill_value=0)
        gate_proj = jnp.dot(rows_in, gate_w, preferred_element_type=jnp.float32)
        up_proj = jnp.dot(rows_in, up_w, preferred_element_type=jnp.float32)
        hidden = (jax.nn.silu(gate_proj) * up_proj).astype(jnp.bfloat16)
        return jnp.dot(hidden, down_w, preferred_element_type=jnp.float32)
    expert_out = lax.map(one_expert, (w_gate, w_up, w_down, by_expert))
    source_ids = jnp.arange(N_SP, dtype=jnp.int32)[:, None]
    flat_index = block_ids * (N_SP * CAP) + source_ids * CAP + (positions - block_ids * CAP)
    picked = jnp.take(expert_out.reshape(EXPERTS * N_SP * CAP, D), flat_index.reshape(-1).astype(jnp.int32), axis=0)
    routed = lax.optimization_barrier(jnp.sum((picked * route_weight.reshape(-1, 1)).reshape(TOKENS, TOPK, D), axis=1))
    return (mid_float + routed).astype(jnp.bfloat16)
```

```python
import jax
import jax.numpy as jnp
from jax import lax
from jax.experimental import pallas as pl
from jax.experimental.pallas import tpu as pltpu
from jax.sharding import PartitionSpec as P

DKW = 128
DKN = 64
DV = 64
TOPK = 2
LANES = 128
ROWS = 16
EPS = 1e-06
F32 = jnp.float32
BF16 = jnp.bfloat16


def silu(v):
    return v / (1.0 + jnp.exp(-v))


def dot(a, b):
    return lax.dot_general(a, b, (((1,), (0,)), ((), ())), preferred_element_type=F32)


def dot_nt(a, b):
    return lax.dot_general(a, b, (((1,), (1,)), ((), ())), preferred_element_type=F32)


def remote(src, dst, send, recv, **where):
    return pltpu.make_async_remote_copy(
        src_ref=src,
        dst_ref=dst,
        send_sem=send,
        recv_sem=recv,
        device_id=where,
        device_id_type=pl.DeviceIdType.MESH,
    )


def greet(n_sp, n_tp, sp, tp):
    barrier = pltpu.get_barrier_semaphore()
    for d in range(1, n_sp):
        pl.semaphore_signal(
            barrier,
            inc=1,
            device_id={"sp": lax.rem(sp + d, n_sp)},
            device_id_type=pl.DeviceIdType.MESH,
        )
    for d in range(1, n_tp):
        pl.semaphore_signal(
            barrier,
            inc=1,
            device_id={"tp": lax.rem(tp + d, n_tp)},
            device_id_type=pl.DeviceIdType.MESH,
        )
    return barrier


def front_kernel(
    n_sp,
    n_tp,
    qw,
    qn,
    fw,
    fn,
    rw,
    rn,
    values,
    gate,
    gain,
    w_out,
    residual,
    norm_gain,
    pick,
    mid_out,
    rows_out,
    pack,
    partner,
    chip,
    chips,
    half_in,
    half_got,
    state_in,
    far_q,
    local_out,
    mixed,
    mixbuf,
    squares,
    sqbuf,
    outgoing,
    psem,
    csem,
    crem,
    hsem,
    msem,
    mrem,
    qsem,
    qrem,
    asem,
    arem,
    fsem,
    frem,
):
    sp = lax.axis_index("sp")
    tp = lax.axis_index("tp")
    barrier = greet(n_sp, n_tp, sp, tp)
    length = qw.shape[0]
    wide = qw.shape[1]
    lanes = wide + qn.shape[1]
    pairs = wide // DKW
    cols = residual.shape[1]
    cap = rows_out.shape[0] // n_sp
    n_z = n_sp // 2
    core = lax.rem(sp, 2)
    z = sp // 2

    row = lax.broadcasted_iota(jnp.int32, (length, length), 0)
    col = lax.broadcasted_iota(jnp.int32, (length, length), 1)
    causal = row >= col
    tri = jnp.where(causal, 1.0, 0.0).astype(BF16)
    low = lax.broadcasted_iota(jnp.int32, (1, LANES), 1) < DV

    def prepare(q_ref, f_ref, room_ref, at):
        q = silu(q_ref[:, at].astype(F32))
        rate = room_ref[:, at] / (1.0 + jnp.exp(f_ref[:, at].astype(F32)))
        log = jnp.log1p(-rate)
        high = log.astype(BF16)
        inside = dot(tri, high) + dot(tri, (log - high.astype(F32)).astype(BF16))
        middle = inside[length // 2 - 1 : length // 2]
        ending = inside[length - 1 : length]
        up = jnp.exp(inside - middle)
        near_q = q * up
        near_r = (rate * jnp.exp(middle - inside)).astype(BF16)
        return (
            near_q,
            near_r,
            (q * jnp.exp(inside)).astype(BF16),
            (rate * jnp.exp(ending - inside)).astype(BF16),
            jnp.exp(ending),
        )

    group_sets = []
    for g in range((lanes - wide) // LANES):
        at = slice(g * LANES, (g + 1) * LANES)
        group_sets.append(prepare(qn, fn, rn, at))
    narrow_states = [None] * len(group_sets)
    for p in range(pairs):
        at = slice(p * LANES, (p + 1) * LANES)
        v = values[:, at]
        v_t = v.astype(F32).T.astype(BF16)
        near_q, near_r, fq, fr, fade = prepare(qw, fw, rw, at)
        scores = jnp.where(causal, dot_nt(near_q.astype(BF16), near_r), 0.0).astype(BF16)
        wide_out = dot(scores, v)
        far_q[:, at] = fq
        pack[:DV, at] = dot(v_t, fr)[:DV].astype(BF16)
        pack[DV:, at] = jnp.broadcast_to(fade, (ROWS, LANES)).astype(BF16)
        near_q, near_r, fq, fr, fade = group_sets[p // 2]
        mine = low if p % 2 == 0 else ~low
        scores = dot_nt(jnp.where(mine, near_q, 0.0).astype(BF16), near_r)
        narrow_out = dot(jnp.where(causal, scores, 0.0).astype(BF16), v)
        local_out[:, at] = jnp.where(low, wide_out, narrow_out)
        piece = jnp.where(mine, dot(v_t, fr)[DV:], 0.0)
        held = narrow_states[p // 2]
        narrow_states[p // 2] = piece if held is None else held + piece
    for g, (_, _, fq, _, fade) in enumerate(group_sets):
        at = slice(wide + g * LANES, wide + (g + 1) * LANES)
        far_q[:, at] = fq
        pack[:DV, at] = narrow_states[g].astype(BF16)
        pack[DV:, at] = jnp.broadcast_to(fade, (ROWS, LANES)).astype(BF16)

    pl.semaphore_wait(barrier, n_sp - 1 + n_tp - 1)
    other = sp + 1 - 2 * core
    to_partner = remote(pack, partner, psem.at[0], psem.at[1], sp=other)
    to_partner.start()
    to_partner.wait()
    half = lanes // 2
    mine = pl.ds(pl.multiple_of(core * half, LANES), half)
    theirs = pl.ds(pl.multiple_of((1 - core) * half, LANES), half)
    own = pack[:, mine].astype(F32)
    far = partner[:, mine].astype(F32)
    first = jnp.where(core == 0, own, far)
    second = jnp.where(core == 0, far, own)
    chip[:DV, :] = (second[DV : DV + 1] * first[:DV] + second[:DV]).astype(BF16)
    chip[DV:, :] = (second[DV:] * first[DV:]).astype(BF16)

    def chip_copy(d):
        return remote(
            chip, chips.at[z], csem.at[d], crem.at[d], sp=lax.rem(z + d, n_z) * 2 + core
        )

    for d in range(1, n_z):
        chip_copy(d).start()
    chips[z] = chip[...]
    for d in range(1, n_z):
        chip_copy(d).wait()
    total = jnp.zeros((DV, half), F32)
    for s in range(n_z):
        piece = chips[s].astype(F32)
        total = jnp.where(s < z, piece[DV : DV + 1] * total + piece[:DV], total)
    half_in[...] = total
    to_partner = remote(half_in, half_got, hsem.at[0], hsem.at[1], sp=other)
    to_partner.start()
    to_partner.wait()

    def enter(part, at):
        prior = partner[:, at].astype(F32)
        moved = prior[DV : DV + 1] * part + prior[:DV]
        state_in[:, at] = jnp.where(core == 1, moved, part).astype(BF16)

    enter(total, mine)
    enter(half_got[...], theirs)

    blank = jnp.zeros((DV, LANES), BF16)
    for p in range(pairs):
        at = slice(p * LANES, (p + 1) * LANES)
        g_at = slice(wide + p // 2 * LANES, wide + (p // 2 + 1) * LANES)
        keep = low if p % 2 == 0 else ~low
        narrow = jnp.where(keep, state_in[:, g_at], jnp.zeros((), BF16))
        out = local_out[:, at]
        out = out + dot_nt(far_q[:, at], jnp.concatenate([state_in[:, at], blank], axis=0))
        out = out + dot_nt(far_q[:, g_at], jnp.concatenate([blank, narrow], axis=0))
        sq = out * out
        wide_mean = jnp.sum(jnp.where(low, sq, 0.0), axis=1, keepdims=True) / DV
        narrow_mean = jnp.sum(jnp.where(low, 0.0, sq), axis=1, keepdims=True) / DV
        scale = lax.rsqrt(jnp.where(low, wide_mean, narrow_mean) + EPS)
        mixed[:, at] = (out * scale * gain[:, at] * silu(gate[:, at].astype(F32))).astype(BF16)

    width = mixed.shape[1]

    def mix_copy(d):
        return remote(mixed, mixbuf.at[d], msem.at[d], mrem.at[d], tp=lax.rem(tp + d, n_tp))

    for d in range(1, n_tp):
        mix_copy(d).start()

    def weight_rows(owner):
        return w_out[pl.ds(pl.multiple_of(owner * width, LANES), width), :]

    acc = residual[...].astype(F32)
    proj = dot(mixed[...], weight_rows(tp))
    for d in range(1, n_tp):
        mix_copy(d).wait()
        proj = proj + dot(mixbuf[d], weight_rows(lax.rem(tp + n_tp - d, n_tp)))
    mid = (acc + proj).astype(BF16)
    mid_out[...] = mid
    mid = mid.astype(F32)
    squares[...] = jnp.broadcast_to(jnp.sum(mid * mid, axis=1, keepdims=True), squares.shape)

    def sq_copy(d):
        return remote(squares, sqbuf.at[d], qsem.at[d], qrem.at[d], tp=lax.rem(tp + d, n_tp))

    for d in range(1, n_tp):
        sq_copy(d).start()
    total_sq = squares[...]
    for d in range(1, n_tp):
        sq_copy(d).wait()
        total_sq = total_sq + sqbuf[d]
    scale = lax.rsqrt(total_sq[:, :1] / (cols * n_tp) + EPS)
    normed = (mid * scale * norm_gain[...]).astype(BF16)
    outgoing[...] = dot(pick[...], normed).astype(BF16)

    def block(ref, owner, width_at):
        return ref.at[pl.ds(pl.multiple_of(owner * cap, ROWS), cap), width_at]

    here = pl.ds(pl.multiple_of(tp * cols, LANES), cols)
    whole = slice(None)

    def send_copy(d):
        peer = lax.rem(sp + d, n_sp)
        return remote(
            block(outgoing, peer, whole), block(rows_out, sp, here), asem.at[d], arem.at[d], sp=peer
        )

    def forward_copy(d, k):
        place = block(rows_out, lax.rem(sp + n_sp - d, n_sp), here)
        return remote(place, place, fsem.at[d, k], frem.at[d, k], tp=lax.rem(tp + k, n_tp))

    def own_copy(k):
        return remote(
            block(outgoing, sp, whole),
            block(rows_out, sp, here),
            fsem.at[0, k],
            frem.at[0, k],
            tp=lax.rem(tp + k, n_tp),
        )

    def start_send(d, carry):
        send_copy(d).start()
        return carry

    lax.fori_loop(1, n_sp, start_send, 0)
    for k in range(1, n_tp):
        own_copy(k).start()
    mine_rows = pl.ds(pl.multiple_of(sp * cap, ROWS), cap)
    rows_out[mine_rows, here] = outgoing[mine_rows, :]

    def pass_on(d, carry):
        send_copy(d).wait_recv()
        for k in range(1, n_tp):
            forward_copy(d, k).start()
        return carry

    lax.fori_loop(1, n_sp, pass_on, 0)

    def finish(d, carry):
        send_copy(d).wait_send()
        for k in range(1, n_tp):
            forward_copy(d, k).wait()
        return carry

    for k in range(1, n_tp):
        own_copy(k).wait()
    lax.fori_loop(1, n_sp, finish, 0)


def back_kernel(
    n_sp, n_tp, part, high, low, mid, out, pieces, summed, returned, rsem, rrem, bsem, brem
):
    sp = lax.axis_index("sp")
    tp = lax.axis_index("tp")
    barrier = greet(n_sp, n_tp, sp, tp)
    cols = mid.shape[1]
    cap = part.shape[0] // n_sp
    pl.semaphore_wait(barrier, n_sp - 1 + n_tp - 1)

    def rows_of(d):
        return pl.ds(pl.multiple_of(lax.rem(sp + d, n_sp) * cap, ROWS), cap)

    def cols_of(owner):
        return pl.ds(pl.multiple_of(owner * cols, LANES), cols)

    def reduce_copy(d, k):
        peer = lax.rem(tp + k, n_tp)
        return remote(
            part.at[rows_of(d), cols_of(peer)],
            pieces.at[k - 1, rows_of(d), :],
            rsem.at[d, k],
            rrem.at[d, k],
            tp=peer,
        )

    def start_reduce(d, carry):
        for k in range(1, n_tp):
            reduce_copy(lax.rem(d, n_sp), k).start()
        return carry

    lax.fori_loop(1, n_sp + 1, start_reduce, 0)

    def back_copy(d):
        peer = lax.rem(sp + d, n_sp)
        return remote(
            summed.at[rows_of(d), :],
            returned.at[rows_of(0), :],
            bsem.at[d],
            brem.at[d],
            sp=peer,
        )

    def add_up(d):
        total = part[rows_of(d), cols_of(tp)].astype(F32)
        for k in range(1, n_tp):
            reduce_copy(d, k).wait_recv()
            total = total + pieces[k - 1, rows_of(d), :].astype(F32)
        return total.astype(BF16)

    def pass_back(d, carry):
        summed[rows_of(d), :] = add_up(d)
        back_copy(d).start()
        return carry

    lax.fori_loop(1, n_sp, pass_back, 0)
    returned[rows_of(0), :] = add_up(0)

    def finish(d, carry):
        back_copy(d).wait()
        return carry

    lax.fori_loop(1, n_sp, finish, 0)

    def drain(d, carry):
        for k in range(1, n_tp):
            reduce_copy(d, k).wait_send()
        return carry

    lax.fori_loop(0, n_sp, drain, 0)
    rows = returned[...]
    moe = dot(high[...], rows) + dot(low[...], rows)
    out[...] = (mid[...].astype(F32) + moe).astype(BF16)


def vmem(count):
    return [pl.BlockSpec(memory_space=pltpu.VMEM)] * count


def body(
    residual_in,
    query_wide,
    narrow_head_query,
    forget_wide,
    forget_narrow,
    room_wide,
    room_narrow,
    values,
    out_gate,
    head_gain,
    w_out,
    norm_gain,
    route_ids,
    route_weight,
    w_gate,
    w_up,
    w_down,
):
    n_sp = lax.axis_size("sp")
    n_tp = lax.axis_size("tp")
    length, cols = residual_in.shape
    model = cols * n_tp
    width = values.shape[1]
    capacity = (7 * TOPK * length + 6 * n_sp - 1) // (6 * n_sp)
    cap = -(-capacity // ROWS) * ROWS
    slots = n_sp * cap
    room_narrow = room_narrow[None]
    narrow = room_narrow.shape[1]
    fill = -narrow % LANES
    if fill:
        edge = ((0, 0), (0, fill))
        narrow_head_query = jnp.pad(narrow_head_query, edge)
        forget_narrow = jnp.pad(forget_narrow, edge)
        room_narrow = jnp.pad(room_narrow, edge)
    lanes = query_wide.shape[1] + narrow + fill

    slot = jnp.arange(slots, dtype=jnp.int32)
    hits = route_ids[:, :, None] == (slot // cap)[None, None, :]
    named = jnp.any(hits, axis=1)
    weight = jnp.sum(jnp.where(hits, route_weight[:, :, None], 0.0), axis=1)
    earlier = jnp.tril(jnp.ones((length, length), BF16), -1)
    rank = jnp.dot(earlier, named.astype(BF16), preferred_element_type=F32)
    placed = named & (rank.astype(jnp.int32) == (slot % cap)[None, :])
    pick = placed.astype(BF16).T
    weight = jnp.where(placed, weight, 0.0)
    high = weight.astype(BF16)
    low = (weight - high.astype(F32)).astype(BF16)

    dma = pltpu.SemaphoreType.DMA
    depth = DV + ROWS
    n_z = n_sp // 2
    mid, rows = pl.pallas_call(
        lambda *refs: front_kernel(n_sp, n_tp, *refs),
        out_shape=(
            jax.ShapeDtypeStruct((length, cols), BF16),
            jax.ShapeDtypeStruct((slots, model), BF16),
        ),
        in_specs=vmem(13),
        out_specs=tuple(vmem(2)),
        scratch_shapes=[
            pltpu.VMEM((depth, lanes), BF16),
            pltpu.VMEM((depth, lanes), BF16),
            pltpu.VMEM((depth, lanes // 2), BF16),
            pltpu.VMEM((n_z, depth, lanes // 2), BF16),
            pltpu.VMEM((DV, lanes // 2), F32),
            pltpu.VMEM((DV, lanes // 2), F32),
            pltpu.VMEM((DV, lanes), BF16),
            pltpu.VMEM((length, lanes), BF16),
            pltpu.VMEM((length, width), F32),
            pltpu.VMEM((length, width), BF16),
            pltpu.VMEM((n_tp, length, width), BF16),
            pltpu.VMEM((length, LANES), F32),
            pltpu.VMEM((n_tp, length, LANES), F32),
            pltpu.VMEM((slots, cols), BF16),
            dma((2,)),
            dma((n_z,)),
            dma((n_z,)),
            dma((2,)),
            dma((n_tp,)),
            dma((n_tp,)),
            dma((n_tp,)),
            dma((n_tp,)),
            dma((n_sp,)),
            dma((n_sp,)),
            dma((n_sp, n_tp)),
            dma((n_sp, n_tp)),
        ],
        compiler_params=pltpu.CompilerParams(collective_id=0, has_side_effects=True),
        name="front",
    )(
        query_wide,
        narrow_head_query,
        forget_wide,
        forget_narrow,
        room_wide[None],
        room_narrow,
        values,
        out_gate,
        head_gain[None],
        w_out,
        residual_in,
        norm_gain[None],
        pick,
    )
    gate_proj = jnp.dot(rows, w_gate[0], preferred_element_type=F32)
    up_proj = jnp.dot(rows, w_up[0], preferred_element_type=F32)
    hidden = (jax.nn.silu(gate_proj) * up_proj).astype(BF16)
    part = jnp.dot(hidden, w_down[0], preferred_element_type=F32).astype(BF16)
    return pl.pallas_call(
        lambda *refs: back_kernel(n_sp, n_tp, *refs),
        out_shape=jax.ShapeDtypeStruct((length, cols), BF16),
        in_specs=vmem(4),
        out_specs=vmem(1)[0],
        scratch_shapes=[
            pltpu.VMEM((n_tp - 1, slots, cols), BF16),
            pltpu.VMEM((slots, cols), BF16),
            pltpu.VMEM((slots, cols), BF16),
            dma((n_sp, n_tp)),
            dma((n_sp, n_tp)),
            dma((n_sp,)),
            dma((n_sp,)),
        ],
        compiler_params=pltpu.CompilerParams(collective_id=1, has_side_effects=True),
        name="back",
    )(part, high, low, mid)


def solution(mesh):
    placed = (
        P("sp", "tp"),
        P("sp", "tp"),
        P("sp", "tp"),
        P("sp", "tp"),
        P("sp", "tp"),
        P("tp"),
        P("tp"),
        P("sp", "tp"),
        P("sp", "tp"),
        P("tp"),
        P(None, "tp"),
        P("tp"),
        P("sp", None),
        P("sp", None),
        P("sp", None, "tp"),
        P("sp", None, "tp"),
        P("sp", "tp", None),
    )
    return jax.shard_map(body, mesh=mesh, in_specs=placed, out_specs=P("sp", "tp"), check_vma=False)
```
